32 devices in a mesh: sp: 8 (over z, x), tp: 4 (over y, core).
Axes of the slice: x: 2, y: 2, z: 4, core: 2. Of those that a mesh axis runs over, the one named last changes fastest.
Arguments:
- tokens: bfloat16 [8192, 4096], P('sp'), may hold values from -6 to 6
- input_norm_scale: bfloat16 [4096], replicated, may hold values from 0.099609375 to 1.8984375
- mean_input_weight: bfloat16 [4096, 2048], P('sp', 'tp'), may hold values from -0.09375 to 0.09375
- query_matrix: bfloat16 [4096, 2048], P('sp', 'tp'), may hold values from -0.09375 to 0.09375
- key_matrix: bfloat16 [4096, 2048], P('sp', 'tp'), may hold values from -0.09375 to 0.09375
- value_matrix: bfloat16 [4096, 2048], P('sp', 'tp'), may hold values from -0.09375 to 0.09375
- strength_weight: bfloat16 [4096, 16], P('sp', 'tp'), may hold values from -0.09375 to 0.09375
- decay_input_weight: bfloat16 [4096, 16], P('sp', 'tp'), may hold values from -0.25 to 0.25
- causal_filter_weight: bfloat16 [4, 3, 2048], replicated, may hold values from -3 to 3
- head_decay_logrates: float32 [16], replicated, may hold values from -13.2 to -2.9
- decay_input_shift: float32 [16], replicated, may hold values from -1 to 1
- strength_shift: float32 [16], replicated, may hold values from -5 to -3
- decay_spike: float32 [8192, 16], P('sp', 'tp'), may hold values from -1.3 to 0
- head_norm_scale: bfloat16 [128], replicated, may hold values from 0.099609375 to 1.8984375
- group_mixing_weight: bfloat16 [16, 128, 128], replicated, may hold values from -0.5 to 0.5
- mean_channel_scale: bfloat16 [2048], replicated, may hold values from 0.099609375 to 1.8984375
- mean_output_weight: bfloat16 [2048, 4096], P('tp', 'sp'), may hold values from -0.09375 to 0.09375
- delta_output_weight: bfloat16 [2048, 4096], P('tp', 'sp'), may hold values from -0.09375 to 0.09375
Outputs:
- mixed_out: bfloat16 [8192, 4096], P(('sp', 'tp'))
The draws below stay inside these ranges and needn't reach their ends.
All inputs are finite; a program needn't handle non-finite values.
Results may differ from the reference program's by a relative error of at most 0.015.
Values may be sent and summed in bfloat16 or wider, within the bound.
No kernel may reach another device: no remote copies, remote signals or barrier semaphores. Data moves between devices by JAX's collectives and lax.ppermute only.
A program may use at most 128 MiB of HBM per device.

```python
import jax
import jax.numpy as jnp
from jax import lax

D = 4096
POOL_GROUPS = 16
GROUP_DIM = 128
MIXER_HEADS = 16
HEAD_DIM = 128
CONV = 4
BLOCK = 64
TOK_DEV = 1024
POOL_W = 2048
GDN_W = 2048
SEQUENCE_TOKENS = 8192
N_TP = 4


def draw_head_decay_logrates(key, part):
    ranking = jax.random.permutation(jax.random.fold_in(key, 11), MIXER_HEADS)
    fast_count = MIXER_HEADS // 2
    fast_rate = jax.random.uniform(jax.random.fold_in(key, 12), (MIXER_HEADS,), jnp.float32, jnp.log(0.012), jnp.log(0.035))
    slow_rate = jax.random.uniform(jax.random.fold_in(key, 13), (MIXER_HEADS,), jnp.float32, jnp.log(2e-06), jnp.log(2e-05))
    return jnp.where(ranking < fast_count, fast_rate, slow_rate).astype(jnp.float32)


def draw_decay_spike(key, part):
    block_ids = jnp.arange(SEQUENCE_TOKENS) // TOK_DEV
    block_rates = jnp.exp(jax.random.uniform(jax.random.fold_in(key, 21), (SEQUENCE_TOKENS // TOK_DEV, MIXER_HEADS), jnp.float32, jnp.log(1e-06), jnp.log(2e-05)))
    stable_portion = -block_rates[block_ids]
    spike_rows = jax.random.randint(jax.random.fold_in(key, 22), (2, MIXER_HEADS), 0, SEQUENCE_TOKENS)
    error_values = jax.random.uniform(jax.random.fold_in(key, 23), (2, MIXER_HEADS), jnp.float32, 0.2, 0.45)
    match_flags = jnp.arange(SEQUENCE_TOKENS)[:, None, None] == spike_rows[None, :, :]
    spike_portion = jnp.sum(jnp.where(match_flags, jnp.log(1.0 - error_values)[None, :, :], 0.0), axis=1)
    return (stable_portion + spike_portion).astype(jnp.float32)


def block_levels(stream_key, dims, split, smallest, largest):
    factor_of, own = 1.0, jax.random.fold_in(stream_key, 6)
    for dim, shards_of in split:
        heights = jnp.exp(jax.random.uniform(jax.random.fold_in(own, dim), (shards_of,), jnp.float32, smallest / len(split), largest / len(split)))
        factor_of = factor_of * jnp.repeat(heights, dims[dim] // shards_of).reshape([-1 if axis == dim else 1 for axis in range(len(dims))])
    return factor_of


def bell_draw(own_key, shape, scale, reach, split=(), held_as=jnp.bfloat16):
    drawn = jax.random.normal(own_key, shape, jnp.float32) * scale
    if len(split) > 0:
        drawn = block_levels(own_key, shape, split, -0.22, 0.18) * drawn
    return jnp.clip(drawn, min=-reach, max=reach).astype(held_as)


def setup_inputs(seed: int = 0) -> dict:
    seeds = jax.random.split(jax.random.key(seed), 19)
    return {
        "tokens": bell_draw(seeds[0], (SEQUENCE_TOKENS, D), 1.0, 6.0, ((0, 8),)),
        "input_norm_scale": jnp.clip(1.0 + 0.18 * jax.random.normal(seeds[1], (D,), jnp.float32), 0.099609375, 1.8984375).astype(jnp.bfloat16),
        "mean_input_weight": bell_draw(seeds[2], (D, POOL_W), D ** -0.5, 0.09375, ((0, 8), (1, 4))),
        "query_matrix": bell_draw(seeds[3], (D, GDN_W), D ** -0.5, 0.09375, ((0, 8), (1, 4))),
        "key_matrix": bell_draw(seeds[4], (D, GDN_W), D ** -0.5, 0.09375, ((0, 8), (1, 4))),
        "value_matrix": bell_draw(seeds[5], (D, GDN_W), D ** -0.5, 0.09375, ((0, 8), (1, 4))),
        "strength_weight": bell_draw(seeds[6], (D, MIXER_HEADS), D ** -0.5, 0.09375, ((0, 8), (1, 4))),
        "decay_input_weight": bell_draw(seeds[7], (D, MIXER_HEADS), (D // 9) ** -0.5, 0.25, ((0, 8), (1, 4))),
        "causal_filter_weight": bell_draw(seeds[8], (CONV, 3, GDN_W), CONV ** -0.5, 3.0),
        "head_decay_logrates": draw_head_decay_logrates(jax.random.fold_in(seeds[18], 71), 0),
        "decay_input_shift": jnp.clip(jax.random.uniform(seeds[10], (MIXER_HEADS,), jnp.float32, -1.0, 1.0), -1.0, 1.0),
        "strength_shift": jnp.clip(jax.random.uniform(seeds[11], (MIXER_HEADS,), jnp.float32, -5.0, -3.0), -5.0, -3.0),
        "decay_spike": draw_decay_spike(jax.random.fold_in(seeds[18], 71), 0),
        "head_norm_scale": jnp.clip(1.0 + 0.18 * jax.random.normal(seeds[13], (HEAD_DIM,), jnp.float32), 0.099609375, 1.8984375).astype(jnp.bfloat16),
        "group_mixing_weight": bell_draw(seeds[14], (POOL_GROUPS, GROUP_DIM, GROUP_DIM), GROUP_DIM ** -0.5, 0.5),
        "mean_channel_scale": jnp.clip(1.0 + 0.18 * jax.random.normal(seeds[15], (POOL_W,), jnp.float32), 0.099609375, 1.8984375).astype(jnp.bfloat16),
        "mean_output_weight": bell_draw(seeds[16], (POOL_W, D), (POOL_W + GDN_W) ** -0.5, 0.09375, ((0, 4), (1, 8))),
        "delta_output_weight": bell_draw(seeds[17], (GDN_W, D), (POOL_W + GDN_W) ** -0.5, 0.09375, ((0, 4), (1, 8))),
    }


EPSILON = 1e-06

def scale_rows(values, gain_vec):
    squares = lax.optimization_barrier(jnp.mean(values * values, axis=-1, keepdims=True))
    return values * lax.rsqrt(squares + EPSILON) * gain_vec.astype(jnp.float32)

def unit_rows(values):
    return values * lax.rsqrt(lax.optimization_barrier(jnp.sum(values * values, axis=-1, keepdims=True)) + EPSILON)

def causal_taps(extended, taps, rows_out):
    tap_sum = jnp.zeros((rows_out, taps.shape[1]), jnp.float32)
    for tap_index in range(taps.shape[0]):
        tap_sum = tap_sum + taps[tap_index] * extended[tap_index:tap_index + rows_out]
    return jax.nn.silu(tap_sum)

def pool_means(previous, current, group_ids, positions):
    pool_reach = 15
    rows_out = current.shape[0]
    extended = jnp.concatenate([previous, current], axis=0).astype(jnp.float32)
    window_size = jnp.left_shift(jnp.int32(2), (group_ids % 4).astype(jnp.int32))
    windowed = jnp.zeros(current.shape, jnp.float32)
    for lag_rows in range(pool_reach + 1):
        shifted = extended[pool_reach - lag_rows:pool_reach - lag_rows + rows_out]
        windowed = windowed + jnp.where(lag_rows < window_size[None, :], shifted, 0.0)
    counts = jnp.minimum(positions[:, None] + 1, window_size[None, :]).astype(jnp.float32)
    return (windowed / counts - extended[pool_reach:]).astype(jnp.bfloat16)

def block_terms(query, keys, values, decay_logarithm, beta):
    blocks = keys.shape[0] // BLOCK

    def to_blocks(tensor):
        return jnp.swapaxes(tensor.reshape((blocks, BLOCK) + tensor.shape[1:]), 1, 2)
    query_b = to_blocks(query)
    keys_b = to_blocks(keys)
    values_b = to_blocks(values)
    decay_b = to_blocks(decay_logarithm)
    beta_b = to_blocks(beta)
    cumulative = jnp.cumsum(decay_b, axis=-1)
    positions = jnp.arange(BLOCK)
    causal = positions[:, None] >= positions[None, :]
    strict = positions[:, None] > positions[None, :]
    spread = cumulative[..., :, None] - cumulative[..., None, :]
    weights = jnp.where(causal, jnp.exp(jnp.where(causal, spread, 0.0)), 0.0)
    keys_beta = keys_b * beta_b[..., None]
    values_beta = values_b * beta_b[..., None]
    intersection = jnp.einsum('nhid,nhjd->nhij', keys_beta, keys_b, precision=lax.Precision.HIGHEST)
    lower_part = jnp.where(strict, intersection * weights, 0.0) + jnp.eye(BLOCK, dtype=jnp.float32)
    right_side = jnp.concatenate([values_beta, keys_beta * jnp.exp(cumulative)[..., None]], axis=-1)
    solved = jax.scipy.linalg.solve_triangular(lower_part, right_side, lower=True, unit_diagonal=True)
    value_depth = values.shape[-1]
    update = solved[..., :value_depth]
    project = solved[..., value_depth:]
    scores = jnp.einsum('nhid,nhjd->nhij', query_b, keys_b, precision=lax.Precision.HIGHEST) * weights
    query_dec = query_b * jnp.exp(cumulative)[..., None]
    keys_dec = keys_b * jnp.exp(cumulative[..., -1:] - cumulative)[..., None]
    carry_decay = jnp.exp(cumulative[..., -1])
    return (scores, query_dec, keys_dec, update, project, carry_decay)

def run_blocks(state, terms):

    def advance(carried, inputs):
        scores, query_dec, keys_dec, update, project, carry_decay = inputs
        fresh = update - jnp.einsum('hcd,hde->hce', project, carried, precision=lax.Precision.HIGHEST)
        output = jnp.einsum('hcd,hde->hce', query_dec, carried, precision=lax.Precision.HIGHEST)
        output = output + jnp.einsum('hij,hje->hie', scores, fresh, precision=lax.Precision.HIGHEST)
        carried = carried * carry_decay[:, None, None] + jnp.einsum('hcd,hce->hde', keys_dec, fresh, precision=lax.Precision.HIGHEST)
        return (carried, output)
    final_state, outputs = lax.scan(advance, state, terms)
    return outputs

def reference(tokens, input_norm_scale, mean_input_weight, query_matrix, key_matrix, value_matrix, strength_weight, decay_input_weight, causal_filter_weight, head_decay_logrates, decay_input_shift, strength_shift, decay_spike, head_norm_scale, group_mixing_weight, mean_channel_scale, mean_output_weight, delta_output_weight):
    normed = scale_rows(tokens.astype(jnp.float32), input_norm_scale).astype(jnp.bfloat16)
    pool_raw = jnp.dot(normed.astype(jnp.float32), mean_input_weight.astype(jnp.float32), preferred_element_type=jnp.float32).astype(jnp.bfloat16)
    query_raw = jnp.dot(normed.astype(jnp.float32), query_matrix.astype(jnp.float32), preferred_element_type=jnp.float32).astype(jnp.bfloat16)
    key_raw = jnp.dot(normed.astype(jnp.float32), key_matrix.astype(jnp.float32), preferred_element_type=jnp.float32).astype(jnp.bfloat16)
    value_raw = jnp.dot(normed.astype(jnp.float32), value_matrix.astype(jnp.float32), preferred_element_type=jnp.float32).astype(jnp.bfloat16)
    beta_raw = jnp.dot(normed.astype(jnp.float32), strength_weight.astype(jnp.float32), preferred_element_type=jnp.float32).astype(jnp.bfloat16)
    decay_unshaped = jnp.dot(normed.astype(jnp.float32), decay_input_weight.astype(jnp.float32), preferred_element_type=jnp.float32).astype(jnp.bfloat16)
    qkv_raw = jnp.concatenate([query_raw, key_raw, value_raw], axis=1)
    extended_qkv = jnp.concatenate([jnp.zeros((CONV - 1, 3 * GDN_W), jnp.bfloat16), qkv_raw], axis=0).astype(jnp.float32)
    convolved = causal_taps(extended_qkv, causal_filter_weight.reshape(CONV, 3 * GDN_W).astype(jnp.float32), SEQUENCE_TOKENS)
    query = unit_rows(convolved[:, :GDN_W].reshape(SEQUENCE_TOKENS, MIXER_HEADS, HEAD_DIM)) * HEAD_DIM ** (-0.5)
    keys = unit_rows(convolved[:, GDN_W:2 * GDN_W].reshape(SEQUENCE_TOKENS, MIXER_HEADS, HEAD_DIM))
    values = convolved[:, 2 * GDN_W:].reshape(SEQUENCE_TOKENS, MIXER_HEADS, HEAD_DIM)
    beta = jax.nn.sigmoid(beta_raw.astype(jnp.float32) + strength_shift)
    decay_logarithm = -jnp.exp(head_decay_logrates) * jax.nn.softplus(decay_unshaped.astype(jnp.float32) + decay_input_shift) + decay_spike
    terms = block_terms(query, keys, values, decay_logarithm, beta)
    outputs = run_blocks(jnp.zeros((MIXER_HEADS, HEAD_DIM, HEAD_DIM), jnp.float32), terms)
    delta_rows = jnp.swapaxes(outputs, 1, 2).reshape(SEQUENCE_TOKENS, MIXER_HEADS, HEAD_DIM)
    delta_mixed = scale_rows(delta_rows, head_norm_scale).astype(jnp.bfloat16).reshape(SEQUENCE_TOKENS, GDN_W)
    group_ids = (jnp.arange(POOL_W) // GROUP_DIM).astype(jnp.int32)
    positions = jnp.arange(SEQUENCE_TOKENS).astype(jnp.int32)
    pool_diff = pool_means(jnp.zeros((15, POOL_W), jnp.bfloat16), pool_raw, group_ids, positions)
    pooled = jnp.einsum('tgc,gcd->tgd', pool_diff.astype(jnp.float32).reshape(SEQUENCE_TOKENS, POOL_GROUPS, GROUP_DIM), group_mixing_weight.astype(jnp.float32))
    pool_mixed = (pooled.reshape(SEQUENCE_TOKENS, POOL_W) * mean_channel_scale.astype(jnp.float32)).astype(jnp.bfloat16)
    pool_slice = POOL_W // N_TP
    delta_slice = GDN_W // N_TP
    summed = jnp.zeros((SEQUENCE_TOKENS, D), jnp.float32)
    for shard_index in range(N_TP):
        pool_part = pool_mixed[:, shard_index * pool_slice:(shard_index + 1) * pool_slice]
        delta_part = delta_mixed[:, shard_index * delta_slice:(shard_index + 1) * delta_slice]
        rows_in = jnp.concatenate([pool_part, delta_part], axis=1)
        weight_rows = jnp.concatenate([mean_output_weight[shard_index * pool_slice:(shard_index + 1) * pool_slice], delta_output_weight[shard_index * delta_slice:(shard_index + 1) * delta_slice]], axis=0)
        partial_sum = jnp.dot(rows_in.astype(jnp.float32), weight_rows.astype(jnp.float32), preferred_element_type=jnp.float32).astype(jnp.bfloat16)
        summed = summed + partial_sum.astype(jnp.float32)
    return summed.astype(jnp.bfloat16)
```

```python
import jax
import jax.numpy as jnp
from jax import lax
from jax.experimental import pallas as pl
from jax.experimental.pallas import tpu as pltpu
from jax.sharding import PartitionSpec as P

GROUP_DIM = 128
HEAD_DIM = 128
CONV = 4
CHUNK = 128


EPSILON = 1e-06


def shifted_2(block, axis, distance):
    devices = range(lax.axis_size(axis))
    route = [(i - distance, i) for i in devices if i - distance in devices]
    return lax.ppermute(block, axis, route)


def scale_rows(values, gain_vec):
    squares = jnp.mean(values * values, axis=-1, keepdims=True)
    return values * lax.rsqrt(squares + EPSILON) * gain_vec.astype(jnp.float32)


def unit_rows(values):
    return values * lax.rsqrt(jnp.sum(values * values, axis=-1, keepdims=True) + EPSILON)


def causal_taps(extended, taps, rows_out):
    tap_sum = jnp.zeros((rows_out, taps.shape[1]), jnp.float32)
    for tap_index in range(taps.shape[0]):
        tap_sum = tap_sum + taps[tap_index] * extended[tap_index : tap_index + rows_out]
    return jax.nn.silu(tap_sum)


def pool_means(previous, current, group_ids, positions):
    pool_reach = 15
    rows_out = current.shape[0]
    extended = jnp.concatenate([previous, current], axis=0).astype(jnp.float32)
    window_size = jnp.left_shift(jnp.int32(2), group_ids % 4)
    windowed = jnp.zeros(current.shape, jnp.float32)
    for lag_rows in range(pool_reach + 1):
        shifted = extended[pool_reach - lag_rows : pool_reach - lag_rows + rows_out]
        windowed = windowed + jnp.where(lag_rows < window_size[None, :], shifted, 0.0)
    counts = jnp.minimum(positions[:, None] + 1, window_size[None, :]).astype(jnp.float32)
    return (windowed / counts - extended[pool_reach:]).astype(jnp.bfloat16)


def mxu(left, right, left_dim, right_dim):
    return lax.dot_general(
        left.astype(jnp.bfloat16),
        right.astype(jnp.bfloat16),
        (((left_dim,), (right_dim,)), ((), ())),
        preferred_element_type=jnp.float32,
    )


def delta_kernel(raw_ref, halo_ref, taps_ref, gates_ref, local_ref, reach_ref, maps_ref, ext_ref):
    chunk = raw_ref.shape[0]
    heads, depth = maps_ref.shape[0], maps_ref.shape[1]
    width = heads * depth
    pad = halo_ref.shape[0]
    conv = taps_ref.shape[0]
    step = pl.program_id(0)
    rows = lax.broadcasted_iota(jnp.int32, (chunk, chunk), 0)
    cols = lax.broadcasted_iota(jnp.int32, (chunk, chunk), 1)

    @pl.when(step == 0)
    def _():
        ext_ref[:pad] = halo_ref[...].astype(jnp.float32)
        lane = lax.broadcasted_iota(jnp.int32, (depth, 2 * depth), 1)
        sub = lax.broadcasted_iota(jnp.int32, (depth, 2 * depth), 0)
        for h in range(heads):
            maps_ref[h] = jnp.where(lane == sub, 1.0, 0.0)

    @pl.when(step > 0)
    def _():
        ext_ref[:pad] = ext_ref[chunk : chunk + pad]

    ext_ref[pad:] = raw_ref[...].astype(jnp.float32)

    def taps_of(part, h):
        low = part * width + h * depth
        total = jnp.zeros((chunk, depth), jnp.float32)
        for i in range(conv):
            first = pad - conv + 1 + i
            total = total + (
                taps_ref[i : i + 1, low : low + depth]
                * ext_ref[first : first + chunk, low : low + depth]
            )
        return total / (1.0 + jnp.exp(-total))

    gates = gates_ref[...]
    causal = rows >= cols
    cumul = lax.dot_general(
        jnp.where(causal, 1.0, 0.0),
        gates,
        (((1,), (0,)), ((), ())),
        precision=lax.Precision.HIGHEST,
        preferred_element_type=jnp.float32,
    )
    cumul_t = cumul.T
    hs = range(heads)
    lower, scores, rights, query_dec, keys_dec, carry = [], [], [], [], [], []
    for h in hs:
        query = unit_rows(taps_of(0, h)) * depth ** (-0.5)
        keys = unit_rows(taps_of(1, h))
        values = taps_of(2, h)
        beta = gates[:, heads + h : heads + h + 1]
        cum = cumul[:, h : h + 1]
        last = cum[chunk - 1 :, :]
        weights = jnp.exp(jnp.where(causal, cum - cumul_t[h : h + 1, :], -1e30))
        keys_16 = keys.astype(jnp.bfloat16)
        lower.append(
            jnp.where(rows > cols, mxu(keys_16, keys_16, 1, 1) * (weights * beta), 0.0)
        )
        scores.append((mxu(query, keys_16, 1, 1) * weights).astype(jnp.bfloat16))
        grown = jnp.exp(cum)
        keys_beta = keys * beta
        rights.append(
            jnp.concatenate([keys_beta * grown, values * beta], axis=1).astype(jnp.bfloat16)
        )
        query_dec.append(query * grown)
        keys_dec.append((keys * jnp.exp(last - cum)).astype(jnp.bfloat16))
        carry.append(jnp.exp(last))
    lower_16 = [x.astype(jnp.bfloat16) for x in lower]
    span = 1
    differ = jnp.bitwise_xor(rows, cols)
    inverse = [jnp.where(rows == cols, 1.0, jnp.where(differ == 1, -x, 0.0)) for x in lower]
    span = 2
    while span < chunk:
        level = jnp.logical_and(differ >= span, differ < 2 * span)
        inner = [
            mxu(jnp.where(level, lower_16[h], jnp.zeros_like(lower_16[h])), inverse[h], 1, 0)
            for h in hs
        ]
        inverse = [inverse[h] - mxu(inverse[h], inner[h], 1, 0) for h in hs]
        span *= 2
    solved = [mxu(inverse[h], rights[h], 1, 0).astype(jnp.bfloat16) for h in hs]
    mixed = [mxu(scores[h], solved[h], 1, 0) for h in hs]
    injects = [mxu(keys_dec[h], solved[h], 0, 0) for h in hs]
    before = [maps_ref[h] for h in hs]
    before_16 = [x.astype(jnp.bfloat16) for x in before]
    reach = [mxu(query_dec[h] - mixed[h][:, :depth], before_16[h], 1, 0) for h in hs]
    moved = [mxu(injects[h][:, :depth], before_16[h], 1, 0) for h in hs]
    for h in hs:
        low = h * depth
        local_ref[:, low : low + depth] = mixed[h][:, depth:] + reach[h][:, depth:]
        reach_ref[:, low : low + depth] = reach[h][:, :depth].astype(jnp.bfloat16)
        after = before[h] * carry[h] - moved[h]
        maps_ref[h, :, :depth] = after[:, :depth]
        maps_ref[h, :, depth:] = after[:, depth:] + injects[h][:, depth:]


def delta_local(raw, halo, taps, gates, heads, depth):
    tok_rows, wide = raw.shape
    chunk = min(CHUNK, tok_rows)
    width = heads * depth
    return pl.pallas_call(
        delta_kernel,
        grid=(tok_rows // chunk,),
        in_specs=[
            pl.BlockSpec((chunk, wide), lambda i: (i, 0)),
            pl.BlockSpec(halo.shape, lambda i: (0, 0)),
            pl.BlockSpec(taps.shape, lambda i: (0, 0)),
            pl.BlockSpec((chunk, gates.shape[1]), lambda i: (i, 0)),
        ],
        out_specs=[
            pl.BlockSpec((chunk, width), lambda i: (i, 0)),
            pl.BlockSpec((chunk, width), lambda i: (i, 0)),
            pl.BlockSpec((heads, depth, 2 * depth), lambda i: (0, 0, 0)),
        ],
        out_shape=[
            jax.ShapeDtypeStruct((tok_rows, width), jnp.float32),
            jax.ShapeDtypeStruct((tok_rows, width), jnp.bfloat16),
            jax.ShapeDtypeStruct((heads, depth, 2 * depth), jnp.float32),
        ],
        scratch_shapes=[pltpu.VMEM((chunk + halo.shape[0], wide), jnp.float32)],
        compiler_params=pltpu.CompilerParams(dimension_semantics=("arbitrary",)),
        cost_estimate=pl.CostEstimate(
            flops=60 * tok_rows * width * chunk, bytes_accessed=10 * tok_rows * width, transcendentals=0
        ),
    )(raw, halo, taps, gates)


def finish_kernel(place_ref, maps_ref, local_ref, reach_ref, gain_ref, out_ref, state_ref):
    count, heads, depth = maps_ref.shape[0], maps_ref.shape[1], maps_ref.shape[2]

    @pl.when(pl.program_id(0) == 0)
    def _():
        place = place_ref[0]
        states = [jnp.zeros((depth, depth), jnp.float32) for h in range(heads)]
        for j in range(count - 1):
            for h in range(heads):
                found = maps_ref[j, h]
                moved = mxu(found[:, :depth], states[h], 1, 0) + found[:, depth:].astype(jnp.float32)
                states[h] = jnp.where(j < place, moved, states[h])
        for h in range(heads):
            state_ref[h] = states[h].astype(jnp.bfloat16)

    for h in range(heads):
        low = h * depth
        rows = local_ref[:, low : low + depth] + mxu(
            reach_ref[:, low : low + depth], state_ref[h], 1, 0
        )
        out_ref[:, low : low + depth] = scale_rows(rows, gain_ref[...]).astype(jnp.bfloat16)


def delta_finish(place, maps, local, reach, gain):
    tok_rows, width = local.shape
    heads, depth = maps.shape[1], maps.shape[2]
    block = min(256, tok_rows)
    return pl.pallas_call(
        finish_kernel,
        grid=(tok_rows // block,),
        in_specs=[
            pl.BlockSpec(memory_space=pltpu.SMEM),
            pl.BlockSpec(maps.shape, lambda i: (0, 0, 0, 0)),
            pl.BlockSpec((block, width), lambda i: (i, 0)),
            pl.BlockSpec((block, width), lambda i: (i, 0)),
            pl.BlockSpec((1, depth), lambda i: (0, 0)),
        ],
        out_specs=pl.BlockSpec((block, width), lambda i: (i, 0)),
        out_shape=jax.ShapeDtypeStruct((tok_rows, width), jnp.bfloat16),
        scratch_shapes=[pltpu.VMEM((heads, depth, depth), jnp.bfloat16)],
        compiler_params=pltpu.CompilerParams(dimension_semantics=("arbitrary",)),
        cost_estimate=pl.CostEstimate(
            flops=4 * tok_rows * width * depth, bytes_accessed=8 * tok_rows * width, transcendentals=0
        ),
    )(place, maps, local, reach, gain)


def per_device(
    tokens,
    input_norm_scale,
    mean_input_weight,
    query_matrix,
    key_matrix,
    value_matrix,
    strength_weight,
    decay_input_weight,
    causal_filter_weight,
    head_decay_logrates,
    decay_input_shift,
    strength_shift,
    decay_spike,
    head_norm_scale,
    group_mixing_weight,
    mean_channel_scale,
    mean_output_weight,
    delta_output_weight,
):
    tok_rows = tokens.shape[0]
    pool_cols = mean_input_weight.shape[1]
    delta_cols = query_matrix.shape[1]
    head_count = strength_weight.shape[1]
    head_depth = delta_cols // head_count
    groups_dev = pool_cols // GROUP_DIM
    tp_index = lax.axis_index("tp")
    sp_index = lax.axis_index("sp")
    normed = scale_rows(tokens.astype(jnp.float32), input_norm_scale).astype(jnp.bfloat16)
    narrow_own = jnp.concatenate([strength_weight, decay_input_weight], axis=1).T
    narrow_part = lax.all_gather(narrow_own, "sp", axis=1, tiled=True)
    qkv_raw = jnp.concatenate(
        [
            jnp.dot(
                normed,
                lax.all_gather(own, "sp", axis=0, tiled=True),
                preferred_element_type=jnp.float32,
            ).astype(jnp.bfloat16)
            for own in (query_matrix, key_matrix, value_matrix)
        ],
        axis=1,
    )
    pool_raw = jnp.dot(
        normed,
        lax.all_gather(mean_input_weight, "sp", axis=0, tiled=True),
        preferred_element_type=jnp.float32,
    ).astype(jnp.bfloat16)
    narrow_sum = mxu(normed, narrow_part, 1, 1)
    beta_raw = narrow_sum[:, :head_count].astype(jnp.bfloat16)
    decay_unshaped = narrow_sum[:, head_count:].astype(jnp.bfloat16)
    pool_reach = 15
    previous_qkv = shifted_2(qkv_raw[tok_rows - 8 :], "sp", 1)
    previous_pool = shifted_2(pool_raw[tok_rows - pool_reach :], "sp", 1)
    conv_local = (
        lax.dynamic_slice_in_dim(causal_filter_weight, tp_index * delta_cols, delta_cols, 2)
        .reshape(CONV, 3 * delta_cols)
        .astype(jnp.float32)
    )
    rate_logarithm = lax.dynamic_slice_in_dim(
        head_decay_logrates, tp_index * head_count, head_count
    )
    shift_amounts = lax.dynamic_slice_in_dim(decay_input_shift, tp_index * head_count, head_count)
    strength_offsets = lax.dynamic_slice_in_dim(strength_shift, tp_index * head_count, head_count)
    beta = jax.nn.sigmoid(beta_raw.astype(jnp.float32) + strength_offsets)
    decay_logarithm = (
        -jnp.exp(rate_logarithm)
        * jax.nn.softplus(decay_unshaped.astype(jnp.float32) + shift_amounts)
        + decay_spike
    )
    gates = jnp.concatenate([decay_logarithm, beta], axis=1)
    gates = jnp.pad(gates, ((0, 0), (0, 128 - 2 * head_count)))
    local_rows, reach, own_maps = delta_local(
        qkv_raw, previous_qkv, conv_local, gates, head_count, head_depth
    )
    maps = lax.all_gather(own_maps.astype(jnp.bfloat16), "sp", axis=0)
    delta_mixed = delta_finish(
        sp_index.reshape(1), maps, local_rows, reach, head_norm_scale.reshape(1, -1)
    )
    group_ids = tp_index * groups_dev + jnp.arange(pool_cols) // GROUP_DIM
    positions = sp_index * tok_rows + jnp.arange(tok_rows)
    pool_diff = pool_means(previous_pool, pool_raw, group_ids, positions)
    local_mix = lax.dynamic_slice_in_dim(group_mixing_weight, tp_index * groups_dev, groups_dev, 0)
    pooled = jnp.einsum(
        "tgc,gcd->tgd",
        pool_diff.reshape(tok_rows, groups_dev, GROUP_DIM),
        local_mix,
        preferred_element_type=jnp.float32,
    )
    pool_scale = lax.dynamic_slice_in_dim(mean_channel_scale, tp_index * pool_cols, pool_cols)
    pool_mixed = (pooled.reshape(tok_rows, pool_cols) * pool_scale.astype(jnp.float32)).astype(
        jnp.bfloat16
    )
    pool_out = jnp.dot(
        pool_mixed,
        lax.all_gather(mean_output_weight, "sp", axis=1, tiled=True),
        preferred_element_type=jnp.float32,
    )
    delta_out = jnp.dot(
        delta_mixed,
        lax.all_gather(delta_output_weight, "sp", axis=1, tiled=True),
        preferred_element_type=jnp.float32,
    )
    return lax.psum_scatter(
        (pool_out + delta_out).astype(jnp.bfloat16), "tp", scatter_dimension=0, tiled=True
    )


def solution(mesh):
    return jax.shard_map(
        per_device,
        mesh=mesh,
        in_specs=(
            P("sp", None),
            P(),
            P("sp", "tp"),
            P("sp", "tp"),
            P("sp", "tp"),
            P("sp", "tp"),
            P("sp", "tp"),
            P("sp", "tp"),
            P(),
            P(),
            P(),
            P(),
            P("sp", "tp"),
            P(),
            P(),
            P(),
            P("tp", "sp"),
            P("tp", "sp"),
        ),
        out_specs=P(("sp", "tp"), None),
        check_vma=False,
    )
```

```python
import functools

import jax
import jax.numpy as jnp
import numpy as np
from jax import lax
from jax.experimental import pallas as pl
from jax.experimental.pallas import tpu as pltpu
from jax.sharding import PartitionSpec as P

GROUP_DIM = 128
HEAD_DIM = 128
CONV = 4
CHUNK = 128


EPSILON = 1e-06


def shifted_2(block, axis, distance):
    devices = range(lax.axis_size(axis))
    route = [(i - distance, i) for i in devices if i - distance in devices]
    return lax.ppermute(block, axis, route)


def scale_rows(values, gain_vec):
    squares = jnp.mean(values * values, axis=-1, keepdims=True)
    return values * lax.rsqrt(squares + EPSILON) * gain_vec.astype(jnp.float32)


def unit_rows(values):
    return values * lax.rsqrt(jnp.sum(values * values, axis=-1, keepdims=True) + EPSILON)


def causal_taps(extended, taps, rows_out):
    tap_sum = jnp.zeros((rows_out, taps.shape[1]), jnp.float32)
    for tap_index in range(taps.shape[0]):
        tap_sum = tap_sum + taps[tap_index] * extended[tap_index : tap_index + rows_out]
    return jax.nn.silu(tap_sum)


def pool_means(previous, current, group_ids, positions):
    pool_reach = 15
    rows_out = current.shape[0]
    extended = jnp.concatenate([previous, current], axis=0).astype(jnp.float32)
    window_size = jnp.left_shift(jnp.int32(2), group_ids % 4)
    windowed = jnp.zeros(current.shape, jnp.float32)
    for lag_rows in range(pool_reach + 1):
        shifted = extended[pool_reach - lag_rows : pool_reach - lag_rows + rows_out]
        windowed = windowed + jnp.where(lag_rows < window_size[None, :], shifted, 0.0)
    counts = jnp.minimum(positions[:, None] + 1, window_size[None, :]).astype(jnp.float32)
    return (windowed / counts - extended[pool_reach:]).astype(jnp.bfloat16)


def mxu(left, right, left_dim, right_dim):
    return lax.dot_general(
        left.astype(jnp.bfloat16),
        right.astype(jnp.bfloat16),
        (((left_dim,), (right_dim,)), ((), ())),
        preferred_element_type=jnp.float32,
    )


def delta_kernel(raw_ref, halo_ref, taps_ref, gates_ref, local_ref, reach_ref, maps_ref, ext_ref):
    chunk = raw_ref.shape[0]
    heads, depth = maps_ref.shape[0], maps_ref.shape[1]
    width = heads * depth
    pad = halo_ref.shape[0]
    conv = taps_ref.shape[0]
    step = pl.program_id(0)
    rows = lax.broadcasted_iota(jnp.int32, (chunk, chunk), 0)
    cols = lax.broadcasted_iota(jnp.int32, (chunk, chunk), 1)

    @pl.when(step == 0)
    def _():
        ext_ref[:pad] = halo_ref[...].astype(jnp.float32)
        lane = lax.broadcasted_iota(jnp.int32, (depth, 2 * depth), 1)
        sub = lax.broadcasted_iota(jnp.int32, (depth, 2 * depth), 0)
        for h in range(heads):
            maps_ref[h] = jnp.where(lane == sub, 1.0, 0.0)

    @pl.when(step > 0)
    def _():
        ext_ref[:pad] = ext_ref[chunk : chunk + pad]

    ext_ref[pad:] = raw_ref[...].astype(jnp.float32)

    def taps_of(part, h):
        low = part * width + h * depth
        total = jnp.zeros((chunk, depth), jnp.float32)
        for i in range(conv):
            first = pad - conv + 1 + i
            total = total + (
                taps_ref[i : i + 1, low : low + depth]
                * ext_ref[first : first + chunk, low : low + depth]
            )
        return total / (1.0 + jnp.exp(-total))

    gates = gates_ref[...]
    causal = rows >= cols
    cumul = lax.dot_general(
        jnp.where(causal, 1.0, 0.0),
        gates,
        (((1,), (0,)), ((), ())),
        precision=lax.Precision.HIGHEST,
        preferred_element_type=jnp.float32,
    )
    cumul_t = cumul.T
    hs = range(heads)
    lower, scores, rights, query_dec, keys_dec, carry = [], [], [], [], [], []
    for h in hs:
        query = unit_rows(taps_of(0, h)) * depth ** (-0.5)
        keys = unit_rows(taps_of(1, h))
        values = taps_of(2, h)
        beta = gates[:, heads + h : heads + h + 1]
        cum = cumul[:, h : h + 1]
        last = cum[chunk - 1 :, :]
        weights = jnp.exp(jnp.where(causal, cum - cumul_t[h : h + 1, :], -1e30))
        keys_16 = keys.astype(jnp.bfloat16)
        lower.append(
            jnp.where(rows > cols, mxu(keys_16, keys_16, 1, 1) * (weights * beta), 0.0)
        )
        scores.append((mxu(query, keys_16, 1, 1) * weights).astype(jnp.bfloat16))
        grown = jnp.exp(cum)
        keys_beta = keys * beta
        rights.append(
            jnp.concatenate([keys_beta * grown, values * beta], axis=1).astype(jnp.bfloat16)
        )
        query_dec.append(query * grown)
        keys_dec.append((keys * jnp.exp(last - cum)).astype(jnp.bfloat16))
        carry.append(jnp.exp(last))
    lower_16 = [x.astype(jnp.bfloat16) for x in lower]
    span = 1
    differ = jnp.bitwise_xor(rows, cols)
    inverse = [jnp.where(rows == cols, 1.0, jnp.where(differ == 1, -x, 0.0)) for x in lower]
    span = 2
    while span < chunk:
        level = jnp.logical_and(differ >= span, differ < 2 * span)
        inner = [
            mxu(jnp.where(level, lower_16[h], jnp.zeros_like(lower_16[h])), inverse[h], 1, 0)
            for h in hs
        ]
        inverse = [inverse[h] - mxu(inverse[h], inner[h], 1, 0) for h in hs]
        span *= 2
    solved = [mxu(inverse[h], rights[h], 1, 0).astype(jnp.bfloat16) for h in hs]
    mixed = [mxu(scores[h], solved[h], 1, 0) for h in hs]
    injects = [mxu(keys_dec[h], solved[h], 0, 0) for h in hs]
    before = [maps_ref[h] for h in hs]
    before_16 = [x.astype(jnp.bfloat16) for x in before]
    reach = [mxu(query_dec[h] - mixed[h][:, :depth], before_16[h], 1, 0) for h in hs]
    moved = [mxu(injects[h][:, :depth], before_16[h], 1, 0) for h in hs]
    for h in hs:
        low = h * depth
        local_ref[:, low : low + depth] = mixed[h][:, depth:] + reach[h][:, depth:]
        reach_ref[:, low : low + depth] = reach[h][:, :depth].astype(jnp.bfloat16)
        after = before[h] * carry[h] - moved[h]
        maps_ref[h, :, :depth] = after[:, :depth]
        maps_ref[h, :, depth:] = after[:, depth:] + injects[h][:, depth:]


def delta_local(raw, halo, taps, gates, heads, depth):
    tok_rows, wide = raw.shape
    chunk = min(CHUNK, tok_rows)
    width = heads * depth
    return pl.pallas_call(
        delta_kernel,
        grid=(tok_rows // chunk,),
        in_specs=[
            pl.BlockSpec((chunk, wide), lambda i: (i, 0)),
            pl.BlockSpec(halo.shape, lambda i: (0, 0)),
            pl.BlockSpec(taps.shape, lambda i: (0, 0)),
            pl.BlockSpec((chunk, gates.shape[1]), lambda i: (i, 0)),
        ],
        out_specs=[
            pl.BlockSpec((chunk, width), lambda i: (i, 0)),
            pl.BlockSpec((chunk, width), lambda i: (i, 0)),
            pl.BlockSpec((heads, depth, 2 * depth), lambda i: (0, 0, 0)),
        ],
        out_shape=[
            jax.ShapeDtypeStruct((tok_rows, width), jnp.float32),
            jax.ShapeDtypeStruct((tok_rows, width), jnp.bfloat16),
            jax.ShapeDtypeStruct((heads, depth, 2 * depth), jnp.float32),
        ],
        scratch_shapes=[pltpu.VMEM((chunk + halo.shape[0], wide), jnp.float32)],
        compiler_params=pltpu.CompilerParams(dimension_semantics=("arbitrary",)),
        cost_estimate=pl.CostEstimate(
            flops=60 * tok_rows * width * chunk, bytes_accessed=10 * tok_rows * width, transcendentals=0
        ),
    )(raw, halo, taps, gates)


def finish_kernel(fast, place_ref, maps_ref, local_ref, reach_ref, gain_ref, out_ref, state_ref):
    count, heads, depth = maps_ref.shape[0], maps_ref.shape[1], maps_ref.shape[2]

    @pl.when(pl.program_id(0) == 0)
    def _():
        place = place_ref[0]
        states = [jnp.zeros((depth, depth), jnp.float32) for h in range(heads)]
        for j in range(count - 1):
            slow = count // fast
            ahead = lax.rem(j // fast - place // fast + slow, slow) * fast
            ahead = ahead + lax.rem(j % fast - lax.rem(place, fast) + fast, fast)
            for h in range(heads):
                found = maps_ref[ahead, h]
                moved = mxu(found[:, :depth], states[h], 1, 0) + found[:, depth:].astype(jnp.float32)
                states[h] = jnp.where(j < place, moved, states[h])
        for h in range(heads):
            state_ref[h] = states[h].astype(jnp.bfloat16)

    for h in range(heads):
        low = h * depth
        rows = local_ref[:, low : low + depth] + mxu(
            reach_ref[:, low : low + depth], state_ref[h], 1, 0
        )
        out_ref[:, low : low + depth] = scale_rows(rows, gain_ref[...]).astype(jnp.bfloat16)


def delta_finish(place, fast, maps, local, reach, gain):
    tok_rows, width = local.shape
    heads, depth = maps.shape[1], maps.shape[2]
    block = min(256, tok_rows)
    return pl.pallas_call(
        functools.partial(finish_kernel, fast),
        grid=(tok_rows // block,),
        in_specs=[
            pl.BlockSpec(memory_space=pltpu.SMEM),
            pl.BlockSpec(maps.shape, lambda i: (0, 0, 0, 0)),
            pl.BlockSpec((block, width), lambda i: (i, 0)),
            pl.BlockSpec((block, width), lambda i: (i, 0)),
            pl.BlockSpec((1, depth), lambda i: (0, 0)),
        ],
        out_specs=pl.BlockSpec((block, width), lambda i: (i, 0)),
        out_shape=jax.ShapeDtypeStruct((tok_rows, width), jnp.bfloat16),
        scratch_shapes=[pltpu.VMEM((heads, depth, depth), jnp.bfloat16)],
        compiler_params=pltpu.CompilerParams(dimension_semantics=("arbitrary",)),
        cost_estimate=pl.CostEstimate(
            flops=4 * tok_rows * width * depth, bytes_accessed=8 * tok_rows * width, transcendentals=0
        ),
    )(place, maps, local, reach, gain)


def fast_size(mesh, axis):
    spread = np.moveaxis(mesh.devices, mesh.axis_names.index(axis), 0)
    line = spread.reshape(spread.shape[0], -1)[:, 0]
    slow = 2 if axis == "sp" else 1
    return sum(1 for d in line if d.coords[slow] == line[0].coords[slow])


def turn(block, axis, fast, slow_step, fast_step):
    size = lax.axis_size(axis)
    slow = size // fast
    route = []
    for i in range(size):
        s, f = divmod(i, fast)
        route.append((i, ((s - slow_step) % slow) * fast + (f - fast_step) % fast))
    return lax.ppermute(block, axis, route)


def ring_line(block, sizes, axis, fast, along_slow):
    count = sizes[0] if along_slow else sizes[1]

    def go(value, sign):
        return turn(value, axis, fast, sign if along_slow else 0, 0 if along_slow else sign)

    found = {0: block}
    if count == 1:
        return [block]
    if count == 2:
        return [block, go(block, 1)]
    up = down = block
    for k in range(1, (count - 1) // 2 + 1):
        up, down = go(up, 1), go(down, -1)
        found[k], found[count - k] = up, down
    if count % 2 == 0:
        half = block.shape[0] // 2
        found[count // 2] = jnp.concatenate([go(up[:half], 1), go(down[half:], -1)], axis=0)
    return [found[k] for k in range(count)]


def grid_gather(block, axis, fast, slow_first):
    sizes = (lax.axis_size(axis) // fast, fast)
    if slow_first:
        line = ring_line(block, sizes, axis, fast, True)
        return [ring_line(one, sizes, axis, fast, False) for one in line]
    line = ring_line(block, sizes, axis, fast, False)
    columns = [ring_line(one, sizes, axis, fast, True) for one in line]
    return [[columns[f][s] for f in range(sizes[1])] for s in range(sizes[0])]


def split_gather(block, axis, fast):
    half = block.shape[0] // 2
    first = grid_gather(block[:half], axis, fast, False)
    second = grid_gather(block[half:], axis, fast, True)
    pairs = [
        jnp.concatenate([a, b], axis=0)
        for row_a, row_b in zip(first, second)
        for a, b in zip(row_a, row_b)
    ]
    return pairs, first[0][-1]


def relative(values, dim, index, fast, sign):
    count = lax.axis_size("sp")
    shape = values.shape
    slow = count // fast
    parts = values.reshape(shape[:dim] + (slow, fast, shape[dim] // count) + shape[dim + 1 :])
    parts = jnp.roll(parts, -sign * (index // fast), axis=dim)
    parts = jnp.roll(parts, -sign * (index % fast), axis=dim + 1)
    return parts.reshape(shape)


def sum_over(partial, axis, fast):
    size = lax.axis_size(axis)
    slow = size // fast
    index = lax.axis_index(axis)
    own_s, own_f = index // fast, index % fast
    parts = partial.reshape(slow, fast, partial.shape[0] // size, partial.shape[1])

    def column(f):
        return lax.dynamic_index_in_dim(parts, f % fast, 1, keepdims=False)

    total = column(own_f).astype(jnp.float32)
    for d in range(1, fast):
        total = total + turn(column(own_f + d), axis, fast, 0, -d).astype(jnp.float32)
    held = total.astype(jnp.bfloat16)

    def row(s):
        return lax.dynamic_index_in_dim(held, s % slow, 0, keepdims=False)

    total = lax.dynamic_index_in_dim(total, own_s, 0, keepdims=False)
    for d in range(1, slow):
        total = total + turn(row(own_s + d), axis, fast, -d, 0).astype(jnp.float32)
    return total.astype(jnp.bfloat16)


def per_device(
    fast_sp,
    fast_tp,
    tokens,
    input_norm_scale,
    mean_input_weight,
    query_matrix,
    key_matrix,
    value_matrix,
    strength_weight,
    decay_input_weight,
    causal_filter_weight,
    head_decay_logrates,
    decay_input_shift,
    strength_shift,
    decay_spike,
    head_norm_scale,
    group_mixing_weight,
    mean_channel_scale,
    mean_output_weight,
    delta_output_weight,
):
    tok_rows = tokens.shape[0]
    pool_cols = mean_input_weight.shape[1]
    delta_cols = query_matrix.shape[1]
    head_count = strength_weight.shape[1]
    head_depth = delta_cols // head_count
    groups_dev = pool_cols // GROUP_DIM
    tp_index = lax.axis_index("tp")
    sp_index = lax.axis_index("sp")
    normed = scale_rows(tokens.astype(jnp.float32), input_norm_scale).astype(jnp.bfloat16)
    narrow_own = jnp.concatenate([strength_weight, decay_input_weight], axis=1).T
    narrow_part = lax.all_gather(narrow_own, "sp", axis=1, tiled=True)
    unit_a = jnp.concatenate([query_matrix, key_matrix], axis=1)
    unit_b = jnp.concatenate([value_matrix, mean_input_weight], axis=1)
    unit_c = jnp.concatenate([mean_output_weight, delta_output_weight], axis=0)
    blocks_a, token_a = split_gather(unit_a, "sp", fast_sp)
    unit_b, token_a = lax.optimization_barrier((unit_b, token_a))
    blocks_b, token_b = split_gather(unit_b, "sp", fast_sp)
    unit_c, blocks_b[-1] = lax.optimization_barrier((unit_c, blocks_b[-1]))
    blocks_c, token_c = split_gather(unit_c, "sp", fast_sp)
    turned = relative(normed, 1, sp_index, fast_sp, 1)
    sum_a = jnp.dot(
        turned, jnp.concatenate(blocks_a, axis=0), preferred_element_type=jnp.float32
    ).astype(jnp.bfloat16)
    sum_b = jnp.dot(
        turned, jnp.concatenate(blocks_b, axis=0), preferred_element_type=jnp.float32
    ).astype(jnp.bfloat16)
    qkv_raw = jnp.concatenate([sum_a, sum_b[:, :delta_cols]], axis=1)
    pool_raw = sum_b[:, delta_cols:]
    narrow_sum = mxu(normed, narrow_part, 1, 1)
    beta_raw = narrow_sum[:, :head_count].astype(jnp.bfloat16)
    decay_unshaped = narrow_sum[:, head_count:].astype(jnp.bfloat16)
    pool_reach = 15
    previous_qkv = shifted_2(qkv_raw[tok_rows - 8 :], "sp", 1)
    previous_pool = shifted_2(pool_raw[tok_rows - pool_reach :], "sp", 1)
    conv_local = (
        lax.dynamic_slice_in_dim(causal_filter_weight, tp_index * delta_cols, delta_cols, 2)
        .reshape(CONV, 3 * delta_cols)
        .astype(jnp.float32)
    )
    rate_logarithm = lax.dynamic_slice_in_dim(
        head_decay_logrates, tp_index * head_count, head_count
    )
    shift_amounts = lax.dynamic_slice_in_dim(decay_input_shift, tp_index * head_count, head_count)
    strength_offsets = lax.dynamic_slice_in_dim(strength_shift, tp_index * head_count, head_count)
    beta = jax.nn.sigmoid(beta_raw.astype(jnp.float32) + strength_offsets)
    decay_logarithm = (
        -jnp.exp(rate_logarithm)
        * jax.nn.softplus(decay_unshaped.astype(jnp.float32) + shift_amounts)
        + decay_spike
    )
    gates = jnp.concatenate([decay_logarithm, beta], axis=1)
    gates = jnp.pad(gates, ((0, 0), (0, 128 - 2 * head_count)))
    local_rows, reach, own_maps = delta_local(
        qkv_raw, previous_qkv, conv_local, gates, head_count, head_depth
    )
    own_maps = own_maps.astype(jnp.bfloat16)
    own_maps = own_maps.reshape(head_count * head_depth, 2 * head_depth)
    maps = [one for row in grid_gather(own_maps, "sp", fast_sp, True) for one in row]
    maps = jnp.stack(maps).reshape(-1, head_count, head_depth, 2 * head_depth)
    delta_mixed = delta_finish(
        sp_index.reshape(1), fast_sp, maps, local_rows, reach, head_norm_scale.reshape(1, -1)
    )
    group_ids = tp_index * groups_dev + jnp.arange(pool_cols) // GROUP_DIM
    positions = sp_index * tok_rows + jnp.arange(tok_rows)
    pool_diff = pool_means(previous_pool, pool_raw, group_ids, positions)
    local_mix = lax.dynamic_slice_in_dim(group_mixing_weight, tp_index * groups_dev, groups_dev, 0)
    pooled = jnp.einsum(
        "tgc,gcd->tgd",
        pool_diff.reshape(tok_rows, groups_dev, GROUP_DIM),
        local_mix,
        preferred_element_type=jnp.float32,
    )
    pool_scale = lax.dynamic_slice_in_dim(mean_channel_scale, tp_index * pool_cols, pool_cols)
    pool_mixed = (pooled.reshape(tok_rows, pool_cols) * pool_scale.astype(jnp.float32)).astype(
        jnp.bfloat16
    )
    mixed = jnp.concatenate([pool_mixed, delta_mixed], axis=1)
    half = len(blocks_c) // 2
    outs = []
    for part in (blocks_c[:half], blocks_c[half:]):
        partial = jnp.dot(
            mixed, jnp.concatenate(part, axis=1), preferred_element_type=jnp.float32
        )
        outs.append(sum_over(partial.astype(jnp.bfloat16), "tp", fast_tp))
    return relative(jnp.concatenate(outs, axis=1), 1, sp_index, fast_sp, -1)


def solution(mesh):
    return jax.shard_map(
        functools.partial(per_device, fast_size(mesh, "sp"), fast_size(mesh, "tp")),
        mesh=mesh,
        in_specs=(
            P("sp", None),
            P(),
            P("sp", "tp"),
            P("sp", "tp"),
            P("sp", "tp"),
            P("sp", "tp"),
            P("sp", "tp"),
            P("sp", "tp"),
            P(),
            P(),
            P(),
            P(),
            P("sp", "tp"),
            P(),
            P(),
            P(),
            P("tp", "sp"),
            P("tp", "sp"),
        ),
        out_specs=P(("sp", "tp"), None),
        check_vma=False,
    )
```

```python
import functools

import jax
import jax.numpy as jnp
import numpy as np
from jax import lax
from jax.experimental import pallas as pl
from jax.experimental.pallas import tpu as pltpu
from jax.sharding import PartitionSpec as P

GROUP_DIM = 128
HEAD_DIM = 128
CONV = 4
CHUNK = 128


EPSILON = 1e-06


def shifted_2(block, axis, distance):
    devices = range(lax.axis_size(axis))
    route = [(i - distance, i) for i in devices if i - distance in devices]
    return lax.ppermute(block, axis, route)


def scale_rows(values, gain_vec):
    squares = jnp.mean(values * values, axis=-1, keepdims=True)
    return values * lax.rsqrt(squares + EPSILON) * gain_vec.astype(jnp.float32)


def unit_rows(values):
    return values * lax.rsqrt(jnp.sum(values * values, axis=-1, keepdims=True) + EPSILON)


def causal_taps(extended, taps, rows_out):
    tap_sum = jnp.zeros((rows_out, taps.shape[1]), jnp.float32)
    for tap_index in range(taps.shape[0]):
        tap_sum = tap_sum + taps[tap_index] * extended[tap_index : tap_index + rows_out]
    return jax.nn.silu(tap_sum)


def pool_means(previous, current, group_ids, positions):
    pool_reach = 15
    rows_out = current.shape[0]
    extended = jnp.concatenate([previous, current], axis=0).astype(jnp.float32)
    window_size = jnp.left_shift(jnp.int32(2), group_ids % 4)
    windowed = jnp.zeros(current.shape, jnp.float32)
    for lag_rows in range(pool_reach + 1):
        shifted = extended[pool_reach - lag_rows : pool_reach - lag_rows + rows_out]
        windowed = windowed + jnp.where(lag_rows < window_size[None, :], shifted, 0.0)
    counts = jnp.minimum(positions[:, None] + 1, window_size[None, :]).astype(jnp.float32)
    return (windowed / counts - extended[pool_reach:]).astype(jnp.bfloat16)


def mxu(left, right, left_dim, right_dim):
    return lax.dot_general(
        left.astype(jnp.bfloat16),
        right.astype(jnp.bfloat16),
        (((left_dim,), (right_dim,)), ((), ())),
        preferred_element_type=jnp.float32,
    )


def delta_kernel(raw_ref, halo_ref, taps_ref, gates_ref, local_ref, reach_ref, maps_ref, ext_ref):
    chunk = raw_ref.shape[0]
    heads, depth = maps_ref.shape[0], maps_ref.shape[1]
    width = heads * depth
    pad = halo_ref.shape[0]
    conv = taps_ref.shape[0]
    step = pl.program_id(0)
    rows = lax.broadcasted_iota(jnp.int32, (chunk, chunk), 0)
    cols = lax.broadcasted_iota(jnp.int32, (chunk, chunk), 1)

    @pl.when(step == 0)
    def _():
        ext_ref[:pad] = halo_ref[...].astype(jnp.float32)
        lane = lax.broadcasted_iota(jnp.int32, (depth, 2 * depth), 1)
        sub = lax.broadcasted_iota(jnp.int32, (depth, 2 * depth), 0)
        for h in range(heads):
            maps_ref[h] = jnp.where(lane == sub, 1.0, 0.0)

    @pl.when(step > 0)
    def _():
        ext_ref[:pad] = ext_ref[chunk : chunk + pad]

    ext_ref[pad:] = raw_ref[...].astype(jnp.float32)

    def taps_of(part, h):
        low = part * width + h * depth
        total = jnp.zeros((chunk, depth), jnp.float32)
        for i in range(conv):
            first = pad - conv + 1 + i
            total = total + (
                taps_ref[i : i + 1, low : low + depth]
                * ext_ref[first : first + chunk, low : low + depth]
            )
        return total / (1.0 + jnp.exp(-total))

    gates = gates_ref[...]
    causal = rows >= cols
    cumul = lax.dot_general(
        jnp.where(causal, 1.0, 0.0),
        gates,
        (((1,), (0,)), ((), ())),
        precision=lax.Precision.HIGHEST,
        preferred_element_type=jnp.float32,
    )
    cumul_t = cumul.T
    hs = range(heads)
    lower, scores, rights, query_dec, keys_dec, carry = [], [], [], [], [], []
    for h in hs:
        query = unit_rows(taps_of(0, h)) * depth ** (-0.5)
        keys = unit_rows(taps_of(1, h))
        values = taps_of(2, h)
        beta = gates[:, heads + h : heads + h + 1]
        cum = cumul[:, h : h + 1]
        last = cum[chunk - 1 :, :]
        weights = jnp.exp(jnp.where(causal, cum - cumul_t[h : h + 1, :], -1e30))
        keys_16 = keys.astype(jnp.bfloat16)
        lower.append(
            jnp.where(rows > cols, mxu(keys_16, keys_16, 1, 1) * (weights * beta), 0.0)
        )
        scores.append((mxu(query, keys_16, 1, 1) * weights).astype(jnp.bfloat16))
        grown = jnp.exp(cum)
        keys_beta = keys * beta
        rights.append(
            jnp.concatenate([keys_beta * grown, values * beta], axis=1).astype(jnp.bfloat16)
        )
        query_dec.append(query * grown)
        keys_dec.append((keys * jnp.exp(last - cum)).astype(jnp.bfloat16))
        carry.append(jnp.exp(last))
    lower_16 = [x.astype(jnp.bfloat16) for x in lower]
    span = 1
    differ = jnp.bitwise_xor(rows, cols)
    inverse = [jnp.where(rows == cols, 1.0, jnp.where(differ == 1, -x, 0.0)) for x in lower]
    span = 2
    while span < chunk:
        level = jnp.logical_and(differ >= span, differ < 2 * span)
        inner = [
            mxu(jnp.where(level, lower_16[h], jnp.zeros_like(lower_16[h])), inverse[h], 1, 0)
            for h in hs
        ]
        inverse = [inverse[h] - mxu(inverse[h], inner[h], 1, 0) for h in hs]
        span *= 2
    solved = [mxu(inverse[h], rights[h], 1, 0).astype(jnp.bfloat16) for h in hs]
    mixed = [mxu(scores[h], solved[h], 1, 0) for h in hs]
    injects = [mxu(keys_dec[h], solved[h], 0, 0) for h in hs]
    before = [maps_ref[h] for h in hs]
    before_16 = [x.astype(jnp.bfloat16) for x in before]
    reach = [mxu(query_dec[h] - mixed[h][:, :depth], before_16[h], 1, 0) for h in hs]
    moved = [mxu(injects[h][:, :depth], before_16[h], 1, 0) for h in hs]
    for h in hs:
        low = h * depth
        local_ref[:, low : low + depth] = mixed[h][:, depth:] + reach[h][:, depth:]
        reach_ref[:, low : low + depth] = reach[h][:, :depth].astype(jnp.bfloat16)
        after = before[h] * carry[h] - moved[h]
        maps_ref[h, :, :depth] = after[:, :depth]
        maps_ref[h, :, depth:] = after[:, depth:] + injects[h][:, depth:]


def delta_local(raw, halo, taps, gates, heads, depth):
    tok_rows, wide = raw.shape
    chunk = min(CHUNK, tok_rows)
    width = heads * depth
    return pl.pallas_call(
        delta_kernel,
        grid=(tok_rows // chunk,),
        in_specs=[
            pl.BlockSpec((chunk, wide), lambda i: (i, 0)),
            pl.BlockSpec(halo.shape, lambda i: (0, 0)),
            pl.BlockSpec(taps.shape, lambda i: (0, 0)),
            pl.BlockSpec((chunk, gates.shape[1]), lambda i: (i, 0)),
        ],
        out_specs=[
            pl.BlockSpec((chunk, width), lambda i: (i, 0)),
            pl.BlockSpec((chunk, width), lambda i: (i, 0)),
            pl.BlockSpec((heads, depth, 2 * depth), lambda i: (0, 0, 0)),
        ],
        out_shape=[
            jax.ShapeDtypeStruct((tok_rows, width), jnp.float32),
            jax.ShapeDtypeStruct((tok_rows, width), jnp.bfloat16),
            jax.ShapeDtypeStruct((heads, depth, 2 * depth), jnp.float32),
        ],
        scratch_shapes=[pltpu.VMEM((chunk + halo.shape[0], wide), jnp.float32)],
        compiler_params=pltpu.CompilerParams(dimension_semantics=("arbitrary",)),
        cost_estimate=pl.CostEstimate(
            flops=60 * tok_rows * width * chunk, bytes_accessed=10 * tok_rows * width, transcendentals=0
        ),
    )(raw, halo, taps, gates)


def finish_kernel(fast, place_ref, maps_ref, local_ref, reach_ref, gain_ref, out_ref, state_ref):
    count, heads, depth = maps_ref.shape[0], maps_ref.shape[1], maps_ref.shape[2]

    @pl.when(pl.program_id(0) == 0)
    def _():
        place = place_ref[0]
        states = [jnp.zeros((depth, depth), jnp.float32) for h in range(heads)]
        for j in range(count - 1):
            slow = count // fast
            ahead = lax.rem(j // fast - place // fast + slow, slow) * fast
            ahead = ahead + lax.rem(j % fast - lax.rem(place, fast) + fast, fast)
            for h in range(heads):
                found = maps_ref[ahead, h]
                moved = mxu(found[:, :depth], states[h], 1, 0) + found[:, depth:].astype(jnp.float32)
                states[h] = jnp.where(j < place, moved, states[h])
        for h in range(heads):
            state_ref[h] = states[h].astype(jnp.bfloat16)

    for h in range(heads):
        low = h * depth
        rows = local_ref[:, low : low + depth] + mxu(
            reach_ref[:, low : low + depth], state_ref[h], 1, 0
        )
        out_ref[:, low : low + depth] = scale_rows(rows, gain_ref[...]).astype(jnp.bfloat16)


def delta_finish(place, fast, maps, local, reach, gain):
    tok_rows, width = local.shape
    heads, depth = maps.shape[1], maps.shape[2]
    block = min(256, tok_rows)
    return pl.pallas_call(
        functools.partial(finish_kernel, fast),
        grid=(tok_rows // block,),
        in_specs=[
            pl.BlockSpec(memory_space=pltpu.SMEM),
            pl.BlockSpec(maps.shape, lambda i: (0, 0, 0, 0)),
            pl.BlockSpec((block, width), lambda i: (i, 0)),
            pl.BlockSpec((block, width), lambda i: (i, 0)),
            pl.BlockSpec((1, depth), lambda i: (0, 0)),
        ],
        out_specs=pl.BlockSpec((block, width), lambda i: (i, 0)),
        out_shape=jax.ShapeDtypeStruct((tok_rows, width), jnp.bfloat16),
        scratch_shapes=[pltpu.VMEM((heads, depth, depth), jnp.bfloat16)],
        compiler_params=pltpu.CompilerParams(dimension_semantics=("arbitrary",)),
        cost_estimate=pl.CostEstimate(
            flops=4 * tok_rows * width * depth, bytes_accessed=8 * tok_rows * width, transcendentals=0
        ),
    )(place, maps, local, reach, gain)


def fast_size(mesh, axis):
    spread = np.moveaxis(mesh.devices, mesh.axis_names.index(axis), 0)
    line = spread.reshape(spread.shape[0], -1)[:, 0]
    slow = 2 if axis == "sp" else 1
    return sum(1 for d in line if d.coords[slow] == line[0].coords[slow])


def turn(block, axis, fast, slow_step, fast_step):
    size = lax.axis_size(axis)
    slow = size // fast
    route = []
    for i in range(size):
        s, f = divmod(i, fast)
        route.append((i, ((s - slow_step) % slow) * fast + (f - fast_step) % fast))
    return lax.ppermute(block, axis, route)


def ring_line(block, sizes, axis, fast, along_slow):
    count = sizes[0] if along_slow else sizes[1]

    def go(value, sign):
        return turn(value, axis, fast, sign if along_slow else 0, 0 if along_slow else sign)

    found = {0: block}
    if count == 1:
        return [block]
    if count == 2:
        return [block, go(block, 1)]
    up = down = block
    for k in range(1, (count - 1) // 2 + 1):
        up, down = go(up, 1), go(down, -1)
        found[k], found[count - k] = up, down
    if count % 2 == 0:
        half = block.shape[0] // 2
        found[count // 2] = jnp.concatenate([go(up[:half], 1), go(down[half:], -1)], axis=0)
    return [found[k] for k in range(count)]


def grid_gather(block, axis, fast, slow_first):
    sizes = (lax.axis_size(axis) // fast, fast)
    if slow_first:
        line = ring_line(block, sizes, axis, fast, True)
        return [ring_line(one, sizes, axis, fast, False) for one in line]
    line = ring_line(block, sizes, axis, fast, False)
    columns = [ring_line(one, sizes, axis, fast, True) for one in line]
    return [[columns[f][s] for f in range(sizes[1])] for s in range(sizes[0])]


def split_gather(block, axis, fast):
    half = block.shape[0] // 2
    first = grid_gather(block[:half], axis, fast, False)
    second = grid_gather(block[half:], axis, fast, True)
    pairs = [
        jnp.concatenate([a, b], axis=0)
        for row_a, row_b in zip(first, second)
        for a, b in zip(row_a, row_b)
    ]
    return pairs, first[0][-1]


def absolute(blocks, index, fast):
    slow = len(blocks) // fast
    parts = jnp.stack(blocks).reshape((slow, fast) + blocks[0].shape)
    parts = jnp.roll(parts, index // fast, axis=0)
    parts = jnp.roll(parts, index % fast, axis=1)
    return parts.reshape((len(blocks),) + blocks[0].shape)


def sum_over(partial, axis, fast):
    size = lax.axis_size(axis)
    slow = size // fast
    index = lax.axis_index(axis)
    own_s, own_f = index // fast, index % fast
    parts = partial.reshape(slow, fast, partial.shape[0] // size, partial.shape[1])

    def column(f):
        return lax.dynamic_index_in_dim(parts, f % fast, 1, keepdims=False)

    total = column(own_f).astype(jnp.float32)
    for d in range(1, fast):
        total = total + turn(column(own_f + d), axis, fast, 0, -d).astype(jnp.float32)
    held = total.astype(jnp.bfloat16)

    def row(s):
        return lax.dynamic_index_in_dim(held, s % slow, 0, keepdims=False)

    total = lax.dynamic_index_in_dim(total, own_s, 0, keepdims=False)
    for d in range(1, slow):
        total = total + turn(row(own_s + d), axis, fast, -d, 0).astype(jnp.float32)
    return total.astype(jnp.bfloat16)


def per_device(
    fast_sp,
    fast_tp,
    tokens,
    input_norm_scale,
    mean_input_weight,
    query_matrix,
    key_matrix,
    value_matrix,
    strength_weight,
    decay_input_weight,
    causal_filter_weight,
    head_decay_logrates,
    decay_input_shift,
    strength_shift,
    decay_spike,
    head_norm_scale,
    group_mixing_weight,
    mean_channel_scale,
    mean_output_weight,
    delta_output_weight,
):
    tok_rows = tokens.shape[0]
    pool_cols = mean_input_weight.shape[1]
    delta_cols = query_matrix.shape[1]
    head_count = strength_weight.shape[1]
    head_depth = delta_cols // head_count
    groups_dev = pool_cols // GROUP_DIM
    tp_index = lax.axis_index("tp")
    sp_index = lax.axis_index("sp")
    normed = scale_rows(tokens.astype(jnp.float32), input_norm_scale).astype(jnp.bfloat16)
    narrow_own = jnp.concatenate([strength_weight, decay_input_weight], axis=1)
    narrow_own = jnp.pad(narrow_own, ((0, 0), (0, 128 - narrow_own.shape[1])))
    unit_a = jnp.concatenate([query_matrix, key_matrix, narrow_own], axis=1)
    unit_b = jnp.concatenate([value_matrix, mean_input_weight], axis=1)
    unit_c = jnp.concatenate([mean_output_weight, delta_output_weight], axis=0)
    blocks_a, token_a = split_gather(unit_a, "sp", fast_sp)
    unit_b, token_a = lax.optimization_barrier((unit_b, token_a))
    blocks_b, token_b = split_gather(unit_b, "sp", fast_sp)
    unit_c, blocks_b[-1] = lax.optimization_barrier((unit_c, blocks_b[-1]))
    blocks_c, token_c = split_gather(unit_c, "sp", fast_sp)
    sum_a = jnp.dot(
        normed, absolute(blocks_a, sp_index, fast_sp).reshape(-1, unit_a.shape[1]), preferred_element_type=jnp.float32
    ).astype(jnp.bfloat16)
    sum_b = jnp.dot(
        normed, absolute(blocks_b, sp_index, fast_sp).reshape(-1, unit_b.shape[1]), preferred_element_type=jnp.float32
    ).astype(jnp.bfloat16)
    qkv_raw = jnp.concatenate([sum_a[:, : 2 * delta_cols], sum_b[:, :delta_cols]], axis=1)
    pool_raw = sum_b[:, delta_cols:]
    narrow_sum = sum_a[:, 2 * delta_cols : 2 * delta_cols + 2 * head_count]
    beta_raw = narrow_sum[:, :head_count].astype(jnp.bfloat16)
    decay_unshaped = narrow_sum[:, head_count:].astype(jnp.bfloat16)
    pool_reach = 15
    previous_qkv = shifted_2(qkv_raw[tok_rows - 8 :], "sp", 1)
    previous_pool = shifted_2(pool_raw[tok_rows - pool_reach :], "sp", 1)
    conv_local = (
        lax.dynamic_slice_in_dim(causal_filter_weight, tp_index * delta_cols, delta_cols, 2)
        .reshape(CONV, 3 * delta_cols)
        .astype(jnp.float32)
    )
    rate_logarithm = lax.dynamic_slice_in_dim(
        head_decay_logrates, tp_index * head_count, head_count
    )
    shift_amounts = lax.dynamic_slice_in_dim(decay_input_shift, tp_index * head_count, head_count)
    strength_offsets = lax.dynamic_slice_in_dim(strength_shift, tp_index * head_count, head_count)
    beta = jax.nn.sigmoid(beta_raw.astype(jnp.float32) + strength_offsets)
    decay_logarithm = (
        -jnp.exp(rate_logarithm)
        * jax.nn.softplus(decay_unshaped.astype(jnp.float32) + shift_amounts)
        + decay_spike
    )
    gates = jnp.concatenate([decay_logarithm, beta], axis=1)
    gates = jnp.pad(gates, ((0, 0), (0, 128 - 2 * head_count)))
    local_rows, reach, own_maps = delta_local(
        qkv_raw, previous_qkv, conv_local, gates, head_count, head_depth
    )
    own_maps = own_maps.astype(jnp.bfloat16)
    own_maps = own_maps.reshape(head_count * head_depth, 2 * head_depth)
    maps = [one for row in grid_gather(own_maps, "sp", fast_sp, True) for one in row]
    maps = jnp.stack(maps).reshape(-1, head_count, head_depth, 2 * head_depth)
    delta_mixed = delta_finish(
        sp_index.reshape(1), fast_sp, maps, local_rows, reach, head_norm_scale.reshape(1, -1)
    )
    group_ids = tp_index * groups_dev + jnp.arange(pool_cols) // GROUP_DIM
    positions = sp_index * tok_rows + jnp.arange(tok_rows)
    pool_diff = pool_means(previous_pool, pool_raw, group_ids, positions)
    local_mix = lax.dynamic_slice_in_dim(group_mixing_weight, tp_index * groups_dev, groups_dev, 0)
    pooled = jnp.einsum(
        "tgc,gcd->tgd",
        pool_diff.reshape(tok_rows, groups_dev, GROUP_DIM),
        local_mix,
        preferred_element_type=jnp.float32,
    )
    pool_scale = lax.dynamic_slice_in_dim(mean_channel_scale, tp_index * pool_cols, pool_cols)
    pool_mixed = (pooled.reshape(tok_rows, pool_cols) * pool_scale.astype(jnp.float32)).astype(
        jnp.bfloat16
    )
    mixed = jnp.concatenate([pool_mixed, delta_mixed], axis=1)
    half = len(blocks_c) // 2
    outs = []
    for part in (blocks_c[:half], blocks_c[half:]):
        partial = jnp.dot(
            mixed, jnp.concatenate(part, axis=1), preferred_element_type=jnp.float32
        )
        outs.append(sum_over(partial.astype(jnp.bfloat16), "tp", fast_tp))
    wide = unit_c.shape[1]
    pieces = [out[:, i : i + wide] for out in outs for i in range(0, out.shape[1], wide)]
    ordered = absolute(pieces, sp_index, fast_sp)
    return jnp.swapaxes(ordered, 0, 1).reshape(pieces[0].shape[0], -1)


def solution(mesh):
    return jax.shard_map(
        functools.partial(per_device, fast_size(mesh, "sp"), fast_size(mesh, "tp")),
        mesh=mesh,
        in_specs=(
            P("sp", None),
            P(),
            P("sp", "tp"),
            P("sp", "tp"),
            P("sp", "tp"),
            P("sp", "tp"),
            P("sp", "tp"),
            P("sp", "tp"),
            P(),
            P(),
            P(),
            P(),
            P("sp", "tp"),
            P(),
            P(),
            P(),
            P("tp", "sp"),
            P("tp", "sp"),
        ),
        out_specs=P(("sp", "tp"), None),
        check_vma=False,
    )
```
